32 devices in a mesh: sp: 4 (over z), fs: 4 (over y, x), tp: 2 (over core).
Axes of the slice: x: 2, y: 2, z: 4, core: 2. Of those that a mesh axis runs over, the one named last changes fastest.
Arguments:
- tokens: bfloat16 [4, 3072, 2048], P('fs', 'sp', 'tp'), may hold values from -6 to 6
- in_gain: float32 [2048], replicated, may hold values from 0.1 to 1.9
- ret_query: bfloat16 [2048, 768], P(None, 'tp'), may hold values from -0.125 to 0.125
- ret_key: bfloat16 [2048, 768], P(None, 'tp'), may hold values from -0.125 to 0.125
- ret_value: bfloat16 [2048, 768], P(None, 'tp'), may hold values from -0.125 to 0.125
- att_query: bfloat16 [2048, 768], P(None, 'tp'), may hold values from -8 to 8
- att_key: bfloat16 [2048, 256], P(None, 'tp'), may hold values from -8 to 8
- att_value: bfloat16 [2048, 256], P(None, 'tp'), may hold values from -0.125 to 0.125
- log_decay: float32 [4, 12, 3072], P('fs', 'tp', 'sp'), may hold values from -1.5 to 0
- ret_gain: float32 [768], P('tp'), may hold values from 0.1 to 1.9
- sink_logit: float32 [12], P('tp'), may hold values from 1 to 5
- retentive_exit_matrix: bfloat16 [768, 2048], P('tp'), may hold values from -0.15625 to 0.15625
- out_att: bfloat16 [768, 2048], P('tp'), may hold values from -0.875 to 0.875
Outputs:
- mixed: bfloat16 [4, 3072, 2048], P('fs', ('sp', 'tp'))
The draws below stay inside these ranges and needn't reach their ends.
All inputs are finite; a program needn't handle non-finite values.
Results may differ from the reference program's by a relative error of at most 0.0085.
Values may be sent and summed in bfloat16 or wider, within the bound.
A program may use at most 128 MiB of HBM per device.

```python
import jax
import jax.numpy as jnp
from jax import lax

D = 2048
HEAD_DIM = 64
RET_HEADS = 12
ATT_HEADS = 12
KV_HEADS = 4
WINDOW = 128
TOK_DEV = 768
SEQ = 3072
BATCH = 4


def paired_heads(key):
    keys = jax.random.split(jax.random.fold_in(key, 5), 2)
    key_weight = jax.random.normal(keys[0], (D, KV_HEADS * HEAD_DIM), jnp.float32) * D ** (-0.5)
    query_weight = jax.random.normal(keys[1], (D, ATT_HEADS * HEAD_DIM), jnp.float32) * D ** (-0.5)
    return (jnp.clip(query_weight, -8.0, 8.0), jnp.clip(key_weight, -8.0, 8.0))


def draw_att_query(key, part):
    return paired_heads(key)[0].astype(jnp.bfloat16)


def draw_att_key(key, part):
    return paired_heads(key)[1].astype(jnp.bfloat16)


def draw_log_decay(key, part):
    keys = jax.random.split(jax.random.fold_in(key, 11), 5)
    keep_share = 0.5
    slow = jax.random.uniform(keys[0], (BATCH, RET_HEADS, 1), jnp.float32) < keep_share
    span = 30.0 * jnp.exp(jax.random.uniform(keys[1], (BATCH, RET_HEADS, 1), jnp.float32) * jnp.log(100.0 / 30.0))
    starting_shift_amount = jnp.where(slow, -jnp.log(10.0) / (4.0 * SEQ), -1.0 / span)
    blocks = SEQ // TOK_DEV
    fading_multiplier = jnp.exp(jax.random.uniform(keys[2], (BATCH, 1, blocks), jnp.float32) * jnp.log(3.0))
    fading_multiplier = jnp.repeat(fading_multiplier, TOK_DEV, axis=2)
    location_numbers = jax.random.randint(keys[3], (BATCH, 3, 1), 0, SEQ)
    objective_numbers = jnp.log(1.0 - jax.random.uniform(keys[4], (BATCH, 3, 1), jnp.float32, 0.2, 0.5))
    element_locations = jnp.arange(SEQ)[None, None, :]
    cluster_sets = jnp.sum(jnp.where(element_locations == location_numbers, objective_numbers, 0.0), axis=1, keepdims=True)
    return (starting_shift_amount * fading_multiplier + cluster_sets).astype(jnp.float32)


def block_scale(key, dims, cuts, least, largest):
    def one(axis_at, shards_of):
        heights = jax.random.uniform(jax.random.fold_in(jax.random.fold_in(key, 6), axis_at), (shards_of,), jnp.float32, least / len(cuts), largest / len(cuts))
        return jnp.repeat(jnp.exp(heights), dims[axis_at] // shards_of).reshape((-1,) + (1,) * (len(dims) - axis_at - 1))

    level = one(*cuts[0])
    for cut in cuts[1:]:
        level = level * one(*cut)
    return level


def gaussian(key, dims, width, reach, pieces=(), held_as=jnp.bfloat16):
    array = jax.random.normal(key, dims, jnp.float32) * width
    if len(pieces) > 0:
        array = block_scale(key, dims, pieces, -0.22, 0.18) * array
    return jnp.clip(array, min=-reach, max=reach).astype(held_as)


def setup_inputs(seed: int = 0) -> dict:
    arg_keys = jax.random.split(jax.random.key(seed), 14)
    tokens = gaussian(arg_keys[0], (BATCH, SEQ, D), 1.0, 6.0, ((0, 4), (1, 4), (2, 2)))
    in_gain = jnp.clip(1.0 + 0.18 * jax.random.normal(arg_keys[1], (D,), jnp.float32), 0.1, 1.9)
    ret_query = gaussian(arg_keys[2], (D, RET_HEADS * HEAD_DIM), D ** -0.5, 0.125, ((1, 2),))
    ret_key = gaussian(arg_keys[3], (D, RET_HEADS * HEAD_DIM), D ** -0.5, 0.125, ((1, 2),))
    ret_value = gaussian(arg_keys[4], (D, RET_HEADS * HEAD_DIM), D ** -0.5, 0.125, ((1, 2),))
    att_query = draw_att_query(jax.random.fold_in(arg_keys[13], 71), 0)
    att_key = draw_att_key(jax.random.fold_in(arg_keys[13], 71), 0)
    att_value = gaussian(arg_keys[7], (D, KV_HEADS * HEAD_DIM), D ** -0.5, 0.125, ((1, 2),))
    log_decay = draw_log_decay(jax.random.fold_in(arg_keys[13], 71), 0)
    ret_gain = jnp.clip(1.0 + 0.18 * jax.random.normal(arg_keys[9], (RET_HEADS * HEAD_DIM,), jnp.float32), 0.1, 1.9)
    sink_logit = jnp.clip(1.0 + 4.0 * jax.random.uniform(arg_keys[10], (ATT_HEADS,), jnp.float32) ** block_scale(arg_keys[10], (ATT_HEADS,), ((0, 2),), -0.2, 0.2), 1.0, 5.0)
    retentive_exit_matrix = gaussian(arg_keys[11], (RET_HEADS * HEAD_DIM, D), (2 * RET_HEADS * HEAD_DIM) ** -0.5, 0.15625, ((0, 2),))
    out_att = gaussian(arg_keys[12], (ATT_HEADS * HEAD_DIM, D), (ATT_HEADS * HEAD_DIM // 16) ** -0.5, 0.875, ((0, 2),))
    return dict(tokens=tokens, in_gain=in_gain, ret_query=ret_query, ret_key=ret_key, ret_value=ret_value, att_query=att_query, att_key=att_key, att_value=att_value, log_decay=log_decay, ret_gain=ret_gain, sink_logit=sink_logit, retentive_exit_matrix=retentive_exit_matrix, out_att=out_att)


EPS = 1e-06

def retention_sequence(query_rows, key_rows, value_rows, log_rates, gain):
    heads = log_rates.shape[0]
    blocks = query_rows.shape[0] // TOK_DEV
    fading_multiplier = HEAD_DIM ** (-0.5)
    shaped_q = query_rows.reshape(blocks, TOK_DEV, heads, HEAD_DIM)
    shaped_k = key_rows.reshape(blocks, TOK_DEV, heads, HEAD_DIM)
    shaped_v = value_rows.reshape(blocks, TOK_DEV, heads, HEAD_DIM)
    shaped_r = log_rates.reshape(heads, blocks, TOK_DEV).transpose(1, 0, 2)
    later = jnp.arange(TOK_DEV)[:, None] >= jnp.arange(TOK_DEV)[None, :]

    def advance(state, inputs):
        block_q, block_k, block_v, block_r = inputs
        cumulative = jnp.cumsum(block_r, axis=1)
        decay = jnp.exp(jnp.where(later[None], cumulative[:, :, None] - cumulative[:, None, :], -jnp.inf))
        query_f = block_q.astype(jnp.float32)
        key_f = block_k.astype(jnp.float32)
        value_f = block_v.astype(jnp.float32)
        weights = (jnp.einsum('thd,shd->hts', query_f, key_f) * fading_multiplier * decay).astype(jnp.bfloat16)
        inner = jnp.einsum('hts,shd->thd', weights.astype(jnp.float32), value_f)
        carried = jnp.einsum('thd,hde->the', query_f, state, precision=lax.Precision.HIGHEST)
        carried = carried * jnp.exp(cumulative).T[:, :, None]
        keyed = key_f * (jnp.exp(cumulative[:, -1:] - cumulative) * fading_multiplier).T[:, :, None]
        own_state = jnp.einsum('shd,she->hde', keyed, value_f, precision=lax.Precision.HIGHEST)
        state = jnp.exp(cumulative[:, -1])[:, None, None] * state + own_state
        return (state, inner + carried)
    start_state = jnp.zeros((heads, HEAD_DIM, HEAD_DIM), jnp.float32)
    _, outputs = lax.scan(advance, start_state, (shaped_q, shaped_k, shaped_v, shaped_r))
    outputs = outputs.reshape(-1, heads, HEAD_DIM)
    normed = outputs * lax.rsqrt(lax.optimization_barrier(jnp.mean(outputs * outputs, axis=-1, keepdims=True)) + EPS)
    return (normed.reshape(-1, heads * HEAD_DIM) * gain).astype(jnp.bfloat16)

def window_attention(query_rows, key_ext, value_ext, first_position, sinks):
    length = query_rows.shape[0]
    blocks = length // WINDOW
    heads_kv = key_ext.shape[1] // HEAD_DIM
    heads = query_rows.shape[1] // HEAD_DIM
    group = heads // heads_kv
    shaped_q = query_rows.astype(jnp.float32).reshape(blocks, WINDOW, heads_kv, group, HEAD_DIM)
    key_block_list = key_ext.astype(jnp.float32).reshape(blocks + 1, WINDOW, heads_kv, HEAD_DIM)
    value_blocks = value_ext.astype(jnp.float32).reshape(blocks + 1, WINDOW, heads_kv, HEAD_DIM)
    key_band = jnp.concatenate([key_block_list[:-1], key_block_list[1:]], axis=1)
    value_band = jnp.concatenate([value_blocks[:-1], value_blocks[1:]], axis=1)
    scores = jnp.einsum('nqhgd,nkhd->hgnqk', shaped_q, key_band) * HEAD_DIM ** (-0.5)
    distance = WINDOW + jnp.arange(WINDOW)[:, None] - jnp.arange(2 * WINDOW)[None, :]
    key_position = first_position - WINDOW + jnp.arange(blocks)[:, None] * WINDOW + jnp.arange(2 * WINDOW)[None, :]
    allowed = ((distance >= 0) & (distance < WINDOW))[None] & (key_position >= 0)[:, None, :]
    scores = jnp.where(allowed, scores, -jnp.inf)
    sink_part = sinks.reshape(heads_kv, group, 1, 1, 1)
    greatest_level = jnp.maximum(lax.optimization_barrier(jnp.max(scores, axis=-1, keepdims=True)), sink_part)
    raised = jnp.exp(scores - greatest_level)
    totals = lax.optimization_barrier(jnp.sum(raised, axis=-1, keepdims=True)) + jnp.exp(sink_part - greatest_level)
    weights = (raised / totals).astype(jnp.bfloat16)
    outputs = jnp.einsum('hgnqk,nkhd->nqhgd', weights.astype(jnp.float32), value_band)
    return outputs.reshape(length, heads * HEAD_DIM).astype(jnp.bfloat16)

def reference(tokens, in_gain, ret_query, ret_key, ret_value, att_query, att_key, att_value, log_decay, ret_gain, sink_logit, retentive_exit_matrix, out_att):
    results = []
    for sequence in range(tokens.shape[0]):
        wide = tokens[sequence].astype(jnp.float32)
        inverse = lax.rsqrt(lax.optimization_barrier(jnp.mean(wide * wide, axis=-1, keepdims=True)) + EPS)
        scaled = (wide * in_gain).astype(jnp.bfloat16)

        def project(weight):
            return (jnp.dot(scaled, weight, preferred_element_type=jnp.float32) * inverse).astype(jnp.bfloat16)
        ret_q = project(ret_query)
        ret_k = project(ret_key)
        ret_v = project(ret_value)
        att_q = project(att_query)
        att_k = project(att_key)
        att_v = project(att_value)
        ret_out = retention_sequence(ret_q, ret_k, ret_v, log_decay[sequence], ret_gain)
        padding = jnp.zeros((WINDOW, att_k.shape[1]), jnp.bfloat16)
        att_out = window_attention(att_q, jnp.concatenate([padding, att_k], axis=0), jnp.concatenate([padding, att_v], axis=0), 0, sink_logit)
        summed = jnp.dot(ret_out, retentive_exit_matrix, preferred_element_type=jnp.float32) + jnp.dot(att_out, out_att, preferred_element_type=jnp.float32)
        results.append(summed.astype(jnp.bfloat16))
    return jnp.stack(results)
```

```python
import functools

import jax
import jax.numpy as jnp
from jax import lax
from jax.experimental import pallas as pl
from jax.experimental.pallas import tpu as pltpu
from jax.sharding import PartitionSpec as P

HEAD_DIM = 64
WINDOW = 128
CHUNK = 128
LANES = 128
TILE = 256
EPS = 1e-06
F32 = jnp.float32
BF16 = jnp.bfloat16
EXACT = lax.Precision.HIGHEST

NT = (((1,), (1,)), ((), ()))
TN = (((0,), (0,)), ((), ()))


def layer(
    n_sp, n_tp, kv_heads,
    tok, gain, rq, rk, rv, aq, ak, av, ld, rgain, sink, wr, wa,
    out,
    xb, wb, acc, pb, inv, ldp, ct, cr, eq, ek, dm, st, ub, msg, inbox,
    hb, hin, wo, oacc,
    tok_sem, w_sem, wo_sem, x_send, x_recv, wo_send, wo_recv,
    h_send, h_recv, m_send, m_recv, halo_send, halo_recv,
):
    tp = lax.axis_index("tp")
    sp = lax.axis_index("sp")
    rows, depth = tok.shape
    ret_w, att_w, kv_w = rq.shape[1], aq.shape[1], ak.shape[1]
    heads = ld.shape[0]
    chunks = rows // CHUNK
    pairs = ret_w // LANES
    att_pairs = att_w // LANES
    att_heads = att_w // HEAD_DIM
    out_rows = rows // n_tp
    model = depth * n_tp
    scale = HEAD_DIM ** (-0.5)

    c_rk, c_rv, c_ak = 0, ret_w, 2 * ret_w
    c_av = c_ak + kv_w
    c_rq = c_av + kv_w
    c_aq = c_rq + ret_w
    width = c_aq + att_w
    parts = ((rk, c_rk), (rv, c_rv), (ak, c_ak), (av, c_av), (rq, c_rq), (aq, c_aq))
    kv_tiles, tiles = c_rq // TILE, width // TILE

    def load_tokens():
        return pltpu.make_async_copy(tok, xb.at[0], tok_sem)

    def load_weight(phase, i):
        owner = lax.rem(tp + phase, n_tp)
        ref, col = parts[i]
        return pltpu.make_async_copy(
            ref.at[pl.ds(owner * depth, depth), :],
            wb.at[phase, :, pl.ds(col, ref.shape[1])],
            w_sem.at[phase, i],
        )

    def load_exit(i):
        ref = (wr, wa)[i]
        return pltpu.make_async_copy(
            ref, wo.at[0, pl.ds(i * ret_w, ref.shape[0]), :], wo_sem.at[i]
        )

    def send_tokens(q):
        return pltpu.make_async_remote_copy(
            src_ref=tok, dst_ref=xb.at[n_tp - q],
            send_sem=x_send.at[q - 1], recv_sem=x_recv.at[n_tp - q - 1],
            device_id={"tp": lax.rem(tp + q, n_tp)}, device_id_type=pl.DeviceIdType.MESH,
        )

    def send_exit(q, i):
        ref = (wr, wa)[i]
        return pltpu.make_async_remote_copy(
            src_ref=ref, dst_ref=wo.at[n_tp - q, pl.ds(i * ret_w, ref.shape[0]), :],
            send_sem=wo_send.at[q - 1, i], recv_sem=wo_recv.at[n_tp - q - 1, i],
            device_id={"tp": lax.rem(tp + q, n_tp)}, device_id_type=pl.DeviceIdType.MESH,
        )

    def send_heads(q, i):
        target = lax.rem(tp + q, n_tp)
        cols = pl.ds(i * ret_w, (ret_w, att_w)[i])
        return pltpu.make_async_remote_copy(
            src_ref=hb.at[pl.ds(target * out_rows, out_rows), cols],
            dst_ref=hin.at[n_tp - q - 1, :, cols],
            send_sem=h_send.at[q - 1, i], recv_sem=h_recv.at[n_tp - q - 1, i],
            device_id={"tp": target}, device_id_type=pl.DeviceIdType.MESH,
        )

    def send_state(q):
        return pltpu.make_async_remote_copy(
            src_ref=msg, dst_ref=inbox.at[q - 1],
            send_sem=m_send.at[q - 1], recv_sem=m_recv.at[q - 1],
            device_id={"sp": lax.rem(sp + q, n_sp)}, device_id_type=pl.DeviceIdType.MESH,
        )

    def send_halo():
        cols = pl.ds(c_ak, 2 * kv_w)
        return pltpu.make_async_remote_copy(
            src_ref=pb.at[pl.ds(rows, WINDOW), cols],
            dst_ref=pb.at[pl.ds(0, WINDOW), cols],
            send_sem=halo_send, recv_sem=halo_recv,
            device_id={"sp": lax.rem(sp + 1, n_sp)}, device_id_type=pl.DeviceIdType.MESH,
        )

    barrier = pltpu.get_barrier_semaphore()
    for q in range(1, n_tp):
        pl.semaphore_signal(
            barrier, inc=1, device_id={"tp": lax.rem(tp + q, n_tp)},
            device_id_type=pl.DeviceIdType.MESH,
        )
    for q in range(1, n_sp):
        pl.semaphore_signal(
            barrier, inc=1, device_id={"sp": lax.rem(sp + q, n_sp)},
            device_id_type=pl.DeviceIdType.MESH,
        )
    load_tokens().start()
    for phase in range(n_tp):
        for i in range(len(parts)):
            load_weight(phase, i).start()

    lane = lax.broadcasted_iota(jnp.int32, (CHUNK, LANES), 1)
    row = lax.broadcasted_iota(jnp.int32, (CHUNK, LANES), 0)
    first_half = lane < HEAD_DIM
    lane1 = lax.broadcasted_iota(jnp.int32, (1, LANES), 1)
    half_masks = (
        jnp.where(lane1 < HEAD_DIM, 1.0, 0.0).astype(BF16),
        jnp.where(lane1 < HEAD_DIM, 0.0, 1.0).astype(BF16),
    )
    same_head = (row < HEAD_DIM) == first_half
    pad_rows = 8

    tri = jnp.where(lane <= row, 1.0, 0.0).astype(F32)
    ldp[...] = jnp.zeros_like(ldp)
    ldp[:heads, :] = ld[...]

    pl.semaphore_wait(barrier, n_tp - 1 + n_sp - 1)
    for q in range(1, n_tp):
        send_tokens(q).start()

    for c in range(chunks):
        span = slice(c * CHUNK, (c + 1) * CHUNK)
        part = ldp[:, span]
        ct[span, :] = lax.dot_general(
            tri, part, NT, precision=EXACT, preferred_element_type=F32
        )
        cr[c] = lax.dot_general(
            part[:pad_rows], tri, NT, precision=EXACT, preferred_element_type=F32
        )

    def decays(c, carry):
        span = pl.ds(pl.multiple_of(c * CHUNK, CHUNK), CHUNK)
        columns = ct[span, :]
        rows_c = cr[c]
        for p in range(pairs):
            wide = [
                jnp.broadcast_to(columns[:, h : h + 1], (CHUNK, LANES))
                for h in (2 * p, 2 * p + 1)
            ]
            mixed = jnp.where(first_half, wide[0], wide[1])
            cols = slice(p * LANES, (p + 1) * LANES)
            eq[span, cols] = jnp.exp(mixed)
            ek[span, cols] = jnp.exp(mixed[CHUNK - 1 :, :] - mixed) * scale
            for e in range(2):
                h = 2 * p + e
                gap = jnp.where(lane <= row, wide[e] - rows_c[h : h + 1, :], -jnp.inf)
                dm[c, h] = jnp.exp(gap) * scale
        return carry

    lax.fori_loop(0, chunks, decays, 0)

    def scaled(phase):
        owner = lax.rem(tp + phase, n_tp)
        factors = gain[owner]

        def one(i, carry):
            span = pl.ds(pl.multiple_of(i * CHUNK, CHUNK), CHUNK)
            x = xb[phase, span, :].astype(F32)
            xb[phase, span, :] = (x * factors).astype(BF16)
            squares = jnp.broadcast_to(
                jnp.sum(x * x, axis=1, keepdims=True), (CHUNK, LANES)
            )
            if phase > 0:
                squares = inv[span, :] + squares
            if phase == n_tp - 1:
                squares = lax.rsqrt(squares / model + EPS)
            inv[span, :] = squares
            return carry

        lax.fori_loop(0, chunks, one, 0)

    def project(phase, low, high):
        def one(n, carry):
            cols = pl.ds(pl.multiple_of(n * TILE, TILE), TILE)
            total = jnp.dot(xb[phase], wb[phase, :, cols], preferred_element_type=F32)
            if phase > 0:
                total = acc[:, cols] + total
            if phase == n_tp - 1:
                wide = jnp.concatenate([inv[...]] * (TILE // LANES), axis=1)
                pb[WINDOW:, cols] = (total * wide).astype(BF16)
            else:
                acc[:, cols] = total
            return carry

        lax.fori_loop(low, high, one, 0)

    load_tokens().wait()
    scaled(0)
    for i in range(4):
        load_weight(0, i).wait()
    project(0, 0, kv_tiles)
    for i in range(4, 6):
        load_weight(0, i).wait()
    for q in range(1, n_tp):
        for i in range(2):
            send_exit(q, i).start()
    for i in range(2):
        load_exit(i).start()
    project(0, kv_tiles, tiles)
    for phase in range(1, n_tp):
        for i in range(6):
            load_weight(phase, i).wait()
        send_tokens(n_tp - phase).wait_recv()
        scaled(phase)
        if phase < n_tp - 1:
            project(phase, 0, tiles)
    project(n_tp - 1, 0, kv_tiles)

    @pl.when(sp + 1 < n_sp)
    def _():
        send_halo().start()

    st[...] = jnp.zeros_like(st)

    def own_state(c, totals):
        span = pl.ds(pl.multiple_of(c * CHUNK, CHUNK), CHUNK)
        here = pl.ds(pl.multiple_of(WINDOW + c * CHUNK, CHUNK), CHUNK)
        after = []
        for p in range(pairs):
            cols = slice(p * LANES, (p + 1) * LANES)
            keys = pb[here, c_rk + p * LANES : c_rk + (p + 1) * LANES].astype(F32)
            values = pb[here, c_rv + p * LANES : c_rv + (p + 1) * LANES]
            keyed = (keys * ek[span, cols]).astype(BF16)
            added = lax.dot_general(keyed, values, TN, preferred_element_type=F32)
            added = jnp.where(same_head, added, 0.0)
            ub[c, p] = added
            fade = eq[span, cols][CHUNK - 1 :, :]
            st[p] = st[p] * fade + added
            after.append(totals[p] * fade)
        return tuple(after)

    totals = lax.fori_loop(
        0, chunks, own_state, tuple(jnp.ones((1, LANES), F32) for _ in range(pairs))
    )
    for p in range(pairs):
        msg[p, :HEAD_DIM, :] = (st[p, :HEAD_DIM, :] + st[p, HEAD_DIM:, :]).astype(BF16)
        coarse = totals[p].astype(BF16)
        fine = (totals[p] - coarse.astype(F32)).astype(BF16)
        row16 = lax.broadcasted_iota(jnp.int32, (16, LANES), 0)
        msg[p, HEAD_DIM:, :] = jnp.where(
            row16 == 0, coarse.astype(F32), jnp.where(row16 == 1, fine.astype(F32), 0.0)
        ).astype(BF16)

    for q in range(1, n_sp):
        @pl.when(sp + q < n_sp)
        def _():
            send_state(q).start()

    project(n_tp - 1, kv_tiles, tiles)

    blocks = rows // WINDOW
    q_at = lax.broadcasted_iota(jnp.int32, (WINDOW, 2 * WINDOW), 0)
    k_at = lax.broadcasted_iota(jnp.int32, (WINDOW, 2 * WINDOW), 1)
    distance = WINDOW + q_at - k_at
    in_window = (distance >= 0) & (distance < WINDOW)

    def attend(i, carry):
        n = blocks - 1 - i

        @pl.when((n == 0) & (sp > 0))
        def _():
            send_halo().wait_recv()

        @pl.when((n == 0) & (sp == 0))
        def _():
            pb[:WINDOW, c_ak : c_ak + 2 * kv_w] = jnp.zeros((WINDOW, 2 * kv_w), BF16)

        lowest = jnp.where((n == 0) & (sp == 0), WINDOW, 0)
        allowed = in_window & (k_at >= lowest)
        band = pl.ds(pl.multiple_of(n * WINDOW, WINDOW), 2 * WINDOW)
        here = pl.ds(pl.multiple_of((n + 1) * WINDOW, WINDOW), WINDOW)
        store = pl.ds(pl.multiple_of(n * WINDOW, WINDOW), WINDOW)
        kinds = {}
        for t in range(kv_w // LANES):
            for name, col in (("k", c_ak), ("v", c_av)):
                plain = pb[band, col + t * LANES : col + (t + 1) * LANES]
                turned = pltpu.roll(plain.astype(F32), HEAD_DIM, 1).astype(BF16)
                kinds[name, t] = (plain, turned)
        scores = []
        picks = []
        for h in range(att_heads):
            p, e = h // 2, h % 2
            g = h * kv_heads // att_heads
            picks.append((g // 2, int(g % 2 != e)))
            query = pb[here, c_aq + p * LANES : c_aq + (p + 1) * LANES] * half_masks[e]
            t, turn = picks[h]
            scores.append(
                lax.dot_general(query, kinds["k", t][turn], NT, preferred_element_type=F32)
            )
        weights = []
        for h in range(att_heads):
            s = jnp.where(allowed, scores[h] * scale, -jnp.inf)
            sink_h = sink[h]
            highest = jnp.maximum(jnp.max(s, axis=1, keepdims=True), sink_h)
            raised = jnp.exp(s - highest)
            total = jnp.sum(raised, axis=1, keepdims=True) + jnp.exp(sink_h - highest)
            weights.append((raised * (1.0 / total)).astype(BF16))
        for p in range(att_pairs):
            left = jnp.concatenate([weights[2 * p], weights[2 * p + 1]], axis=1)
            right = jnp.concatenate(
                [
                    kinds["v", picks[2 * p + e][0]][picks[2 * p + e][1]] * half_masks[e]
                    for e in range(2)
                ],
                axis=0,
            )
            hb[store, ret_w + p * LANES : ret_w + (p + 1) * LANES] = jnp.dot(
                left, right, preferred_element_type=F32
            ).astype(BF16)
        return carry

    lax.fori_loop(0, blocks, attend, 0)
    for q in range(1, n_tp):
        send_heads(q, 1).start()

    st[...] = jnp.zeros_like(st)
    for q in range(n_sp - 1, 0, -1):
        @pl.when(sp >= q)
        def _():
            send_state(q).wait_recv()
            for p in range(pairs):
                part = inbox[q - 1, p].astype(F32)
                fade = part[HEAD_DIM : HEAD_DIM + 1] + part[HEAD_DIM + 1 : HEAD_DIM + 2]
                both = jnp.concatenate([part[:HEAD_DIM]] * 2, axis=0)
                st[p] = st[p] * fade + jnp.where(same_head, both, 0.0)

    ones = jnp.where(same_head, 1.0, 0.0).astype(BF16)
    ones2 = jnp.concatenate([ones, ones], axis=0)

    def retain(c, carry):
        span = pl.ds(pl.multiple_of(c * CHUNK, CHUNK), CHUNK)
        here = pl.ds(pl.multiple_of(WINDOW + c * CHUNK, CHUNK), CHUNK)
        kept = []
        for p in range(pairs):
            cols = slice(p * LANES, (p + 1) * LANES)
            query = pb[here, c_rq + p * LANES : c_rq + (p + 1) * LANES]
            keys = pb[here, c_rk + p * LANES : c_rk + (p + 1) * LANES]
            values = pb[here, c_rv + p * LANES : c_rv + (p + 1) * LANES]
            left = [
                (
                    lax.dot_general(
                        query * half_masks[e], keys, NT, preferred_element_type=F32
                    )
                    * dm[c, 2 * p + e]
                ).astype(BF16)
                for e in range(2)
            ]
            state = st[p]
            faded = eq[span, cols]
            left.append((query.astype(F32) * faded).astype(BF16))
            right = [values * half_masks[0], values * half_masks[1], state.astype(BF16)]
            kept.append(
                jnp.dot(
                    jnp.concatenate(left, axis=1),
                    jnp.concatenate(right, axis=0),
                    preferred_element_type=F32,
                )
            )
            st[p] = state * faded[CHUNK - 1 :, :] + ub[c, p]
        for p in range(pairs):
            cols = slice(p * LANES, (p + 1) * LANES)
            r = kept[p]
            square = r * r
            coarse = square.astype(BF16)
            fine = (square - coarse.astype(F32)).astype(BF16)
            total = jnp.dot(
                jnp.concatenate([coarse, fine], axis=1), ones2, preferred_element_type=F32
            )
            normed = r * lax.rsqrt(total * (1.0 / HEAD_DIM) + EPS)
            hb[span, cols] = (normed * rgain[:, cols]).astype(BF16)
        return carry

    lax.fori_loop(0, chunks, retain, 0)
    for q in range(1, n_tp):
        send_heads(q, 0).start()

    for i in range(2):
        load_exit(i).wait()
    mine = pl.ds(pl.multiple_of(tp * out_rows, out_rows), out_rows)

    def leave(phase):
        def one(n, carry):
            cols = pl.ds(pl.multiple_of(n * TILE, TILE), TILE)
            left = hb[mine, :] if phase == 0 else hin[phase - 1]
            total = jnp.dot(left, wo[phase, :, cols], preferred_element_type=F32)
            if phase > 0:
                total = oacc[:, cols] + total
            if phase == n_tp - 1:
                out[:, cols] = total.astype(BF16)
            else:
                oacc[:, cols] = total
            return carry

        lax.fori_loop(0, model // TILE, one, 0)

    leave(0)
    for phase in range(1, n_tp):
        for i in range(2):
            send_exit(n_tp - phase, i).wait_recv()
            send_heads(n_tp - phase, i).wait_recv()
        leave(phase)

    for q in range(1, n_tp):
        send_tokens(q).wait_send()
        for i in range(2):
            send_exit(q, i).wait_send()
            send_heads(q, i).wait_send()
    for q in range(1, n_sp):
        @pl.when(sp + q < n_sp)
        def _():
            send_state(q).wait_send()

    @pl.when(sp + 1 < n_sp)
    def _():
        send_halo().wait_send()


def shards(n_sp, n_tp, tokens, in_gain, rq, rk, rv, aq, ak, av, log_decay, ret_gain, sink, wr, wa):
    rows, depth = tokens.shape[1:]
    ret_w, att_w, kv_w = rq.shape[1], aq.shape[1], ak.shape[1]
    heads = log_decay.shape[1]
    model = depth * n_tp
    width = 3 * ret_w + att_w + 2 * kv_w
    chunks, pairs = rows // CHUNK, ret_w // LANES
    out_rows = rows // n_tp
    kv_heads = kv_w // HEAD_DIM
    later = max(n_sp - 1, 1)
    others = max(n_tp - 1, 1)
    vmem = pl.BlockSpec(memory_space=pltpu.VMEM)
    hbm = pl.BlockSpec(memory_space=pltpu.HBM)
    smem = pl.BlockSpec(memory_space=pltpu.SMEM)
    dma = pltpu.SemaphoreType.DMA
    result = pl.pallas_call(
        functools.partial(layer, n_sp, n_tp, kv_heads),
        out_shape=jax.ShapeDtypeStruct((out_rows, model), BF16),
        in_specs=[hbm, vmem] + [hbm] * 6 + [vmem, vmem, smem, hbm, hbm],
        out_specs=vmem,
        scratch_shapes=[
            pltpu.VMEM((n_tp, rows, depth), BF16),
            pltpu.VMEM((n_tp, depth, width), BF16),
            pltpu.VMEM((rows, width), F32),
            pltpu.VMEM((WINDOW + rows, width), BF16),
            pltpu.VMEM((rows, LANES), F32),
            pltpu.VMEM((LANES, rows), F32),
            pltpu.VMEM((rows, LANES), F32),
            pltpu.VMEM((chunks, 8, CHUNK), F32),
            pltpu.VMEM((rows, ret_w), F32),
            pltpu.VMEM((rows, ret_w), F32),
            pltpu.VMEM((chunks, heads, CHUNK, CHUNK), F32),
            pltpu.VMEM((pairs, LANES, LANES), F32),
            pltpu.VMEM((chunks, pairs, LANES, LANES), F32),
            pltpu.VMEM((pairs, HEAD_DIM + 16, LANES), BF16),
            pltpu.VMEM((later, pairs, HEAD_DIM + 16, LANES), BF16),
            pltpu.VMEM((rows, ret_w + att_w), BF16),
            pltpu.VMEM((others, out_rows, ret_w + att_w), BF16),
            pltpu.VMEM((n_tp, ret_w + att_w, model), BF16),
            pltpu.VMEM((out_rows, model), F32),
            dma, dma((n_tp, 6)), dma((2,)),
            dma((others,)), dma((others,)),
            dma((others, 2)), dma((others, 2)),
            dma((others, 2)), dma((others, 2)),
            dma((later,)), dma((later,)),
            dma, dma,
        ],
        compiler_params=pltpu.CompilerParams(
            collective_id=0, has_side_effects=True, vmem_limit_bytes=60 * 1024 * 1024
        ),
    )(
        tokens[0], in_gain.reshape(n_tp, 1, depth), rq, rk, rv, aq, ak, av,
        log_decay[0], ret_gain.reshape(1, ret_w), sink, wr, wa,
    )
    return result[None]


def solution(mesh):
    n_sp, n_tp = mesh.shape["sp"], mesh.shape["tp"]
    return jax.shard_map(
        functools.partial(shards, n_sp, n_tp),
        mesh=mesh,
        in_specs=(
            P("fs", "sp", "tp"),
            P(),
            P(None, "tp"),
            P(None, "tp"),
            P(None, "tp"),
            P(None, "tp"),
            P(None, "tp"),
            P(None, "tp"),
            P("fs", "tp", "sp"),
            P("tp"),
            P("tp"),
            P("tp", None),
            P("tp", None),
        ),
        out_specs=P("fs", ("sp", "tp"), None),
        check_vma=False,
    )
```

```python
import functools

import jax
import jax.numpy as jnp
from jax import lax
from jax.experimental import pallas as pl
from jax.experimental.pallas import tpu as pltpu
from jax.sharding import PartitionSpec as P

HEAD_DIM = 64
WINDOW = 128
CHUNK = 128
LANES = 128
TILE = 256
EXIT_TILE = 512
EPS = 1e-06
F32 = jnp.float32
BF16 = jnp.bfloat16
EXACT = lax.Precision.HIGHEST

NT = (((1,), (1,)), ((), ()))
TN = (((0,), (0,)), ((), ()))


def layer(
    n_sp, n_tp, kv_heads,
    tok, gain_in, rq, rk, rv, aq, ak, av, ld_in, rgain, sink, wr, wa,
    out,
    xb, wb, acc, pb, inv, ldp, ct, cr, eq, ek, dm, st, ub, msg, inbox,
    hb, hin, wo, oacc,
    gain, ld, small_sem, tok_sem, w_sem, wo_sem, x_send, x_recv, wo_send, wo_recv,
    h_send, h_recv, m_send, m_recv, halo_send, halo_recv,
):
    tp = lax.axis_index("tp")
    sp = lax.axis_index("sp")
    rows, depth = tok.shape
    ret_w, att_w, kv_w = rq.shape[1], aq.shape[1], ak.shape[1]
    heads = ld_in.shape[0]
    chunks = rows // CHUNK
    pairs = ret_w // LANES
    att_pairs = att_w // LANES
    att_heads = att_w // HEAD_DIM
    out_rows = rows // n_tp
    model = depth * n_tp
    scale = HEAD_DIM ** (-0.5)

    c_rk, c_rv, c_ak = 0, ret_w, 2 * ret_w
    c_av = c_ak + kv_w
    c_rq = c_av + kv_w
    c_aq = c_rq + ret_w
    width = c_aq + att_w
    parts = ((rk, c_rk), (rv, c_rv), (ak, c_ak), (av, c_av), (rq, c_rq), (aq, c_aq))
    kv_tiles, tiles = c_rq // TILE, width // TILE

    def load_tokens():
        return pltpu.make_async_copy(tok, xb.at[0], tok_sem)

    def load_weight(phase, i):
        owner = lax.rem(tp + phase, n_tp)
        ref, col = parts[i]
        return pltpu.make_async_copy(
            ref.at[pl.ds(owner * depth, depth), :],
            wb.at[phase, :, pl.ds(col, ref.shape[1])],
            w_sem.at[phase, i],
        )

    def load_exit(i):
        ref = (wr, wa)[i]
        return pltpu.make_async_copy(
            ref, wo.at[0, pl.ds(i * ret_w, ref.shape[0]), :], wo_sem.at[i]
        )

    def send_tokens(q):
        return pltpu.make_async_remote_copy(
            src_ref=tok, dst_ref=xb.at[n_tp - q],
            send_sem=x_send.at[q - 1], recv_sem=x_recv.at[n_tp - q - 1],
            device_id={"tp": lax.rem(tp + q, n_tp)}, device_id_type=pl.DeviceIdType.MESH,
        )

    def send_exit(q, i):
        ref = (wr, wa)[i]
        return pltpu.make_async_remote_copy(
            src_ref=ref, dst_ref=wo.at[n_tp - q, pl.ds(i * ret_w, ref.shape[0]), :],
            send_sem=wo_send.at[q - 1, i], recv_sem=wo_recv.at[n_tp - q - 1, i],
            device_id={"tp": lax.rem(tp + q, n_tp)}, device_id_type=pl.DeviceIdType.MESH,
        )

    def send_heads(q, i):
        target = lax.rem(tp + q, n_tp)
        cols = pl.ds(i * ret_w, (ret_w, att_w)[i])
        return pltpu.make_async_remote_copy(
            src_ref=hb.at[pl.ds(target * out_rows, out_rows), cols],
            dst_ref=hin.at[n_tp - q - 1, :, cols],
            send_sem=h_send.at[q - 1, i], recv_sem=h_recv.at[n_tp - q - 1, i],
            device_id={"tp": target}, device_id_type=pl.DeviceIdType.MESH,
        )

    def send_state(q):
        return pltpu.make_async_remote_copy(
            src_ref=msg, dst_ref=inbox.at[q - 1],
            send_sem=m_send.at[q - 1], recv_sem=m_recv.at[q - 1],
            device_id={"sp": lax.rem(sp + q, n_sp)}, device_id_type=pl.DeviceIdType.MESH,
        )

    def send_halo():
        cols = pl.ds(c_ak, 2 * kv_w)
        return pltpu.make_async_remote_copy(
            src_ref=pb.at[pl.ds(rows, WINDOW), cols],
            dst_ref=pb.at[pl.ds(0, WINDOW), cols],
            send_sem=halo_send, recv_sem=halo_recv,
            device_id={"sp": lax.rem(sp + 1, n_sp)}, device_id_type=pl.DeviceIdType.MESH,
        )

    rates = pltpu.make_async_copy(ld_in, ld, small_sem.at[0])
    gains = pltpu.make_async_copy(gain_in, gain, small_sem.at[1])
    rates.start()
    gains.start()
    barrier = pltpu.get_barrier_semaphore()
    for q in range(1, n_tp):
        pl.semaphore_signal(
            barrier, inc=1, device_id={"tp": lax.rem(tp + q, n_tp)},
            device_id_type=pl.DeviceIdType.MESH,
        )
    for q in range(1, n_sp):
        pl.semaphore_signal(
            barrier, inc=1, device_id={"sp": lax.rem(sp + q, n_sp)},
            device_id_type=pl.DeviceIdType.MESH,
        )
    load_tokens().start()
    for phase in range(n_tp):
        for i in range(len(parts)):
            load_weight(phase, i).start()

    lane = lax.broadcasted_iota(jnp.int32, (CHUNK, LANES), 1)
    row = lax.broadcasted_iota(jnp.int32, (CHUNK, LANES), 0)
    first_half = lane < HEAD_DIM
    lane1 = lax.broadcasted_iota(jnp.int32, (1, LANES), 1)
    half_masks = (
        jnp.where(lane1 < HEAD_DIM, 1.0, 0.0).astype(BF16),
        jnp.where(lane1 < HEAD_DIM, 0.0, 1.0).astype(BF16),
    )
    same_head = (row < HEAD_DIM) == first_half
    pad_rows = 8

    tri = jnp.where(lane <= row, 1.0, 0.0).astype(F32)
    ldp[...] = jnp.zeros_like(ldp)
    rates.wait()
    for h in range(heads):
        ldp[h : h + 1, :] = ld[h]

    for c in range(chunks):
        span = slice(c * CHUNK, (c + 1) * CHUNK)
        part = ldp[:, span]
        ct[span, :] = lax.dot_general(
            tri, part, NT, precision=EXACT, preferred_element_type=F32
        )
        cr[c] = lax.dot_general(
            part[:pad_rows], tri, NT, precision=EXACT, preferred_element_type=F32
        )

    def decays(c, carry):
        span = pl.ds(pl.multiple_of(c * CHUNK, CHUNK), CHUNK)
        columns = ct[span, :]
        rows_c = cr[c]
        for p in range(pairs):
            wide = [
                jnp.broadcast_to(columns[:, h : h + 1], (CHUNK, LANES))
                for h in (2 * p, 2 * p + 1)
            ]
            mixed = jnp.where(first_half, wide[0], wide[1])
            cols = slice(p * LANES, (p + 1) * LANES)
            eq[span, cols] = jnp.exp(mixed)
            ek[span, cols] = jnp.exp(mixed[CHUNK - 1 :, :] - mixed) * scale
            for e in range(2):
                h = 2 * p + e
                gap = jnp.where(lane <= row, wide[e] - rows_c[h : h + 1, :], -jnp.inf)
                dm[c, h] = jnp.exp(gap) * scale
        return carry

    lax.fori_loop(0, chunks, decays, 0)

    pl.semaphore_wait(barrier, n_tp - 1 + n_sp - 1)
    for q in range(1, n_tp):
        send_tokens(q).start()

    def scaled(phase):
        owner = lax.rem(tp + phase, n_tp)
        factors = gain[owner]

        def one(i, carry):
            span = pl.ds(pl.multiple_of(i * CHUNK, CHUNK), CHUNK)
            x = xb[phase, span, :].astype(F32)
            xb[phase, span, :] = (x * factors).astype(BF16)
            squares = jnp.broadcast_to(
                jnp.sum(x * x, axis=1, keepdims=True), (CHUNK, LANES)
            )
            if phase > 0:
                squares = inv[span, :] + squares
            if phase == n_tp - 1:
                squares = lax.rsqrt(squares / model + EPS)
            inv[span, :] = squares
            return carry

        lax.fori_loop(0, chunks, one, 0)

    def project(phase, low, high):
        def one(n, carry):
            cols = pl.ds(pl.multiple_of(n * TILE, TILE), TILE)
            total = jnp.dot(xb[phase], wb[phase, :, cols], preferred_element_type=F32)
            if phase > 0:
                total = acc[:, cols] + total
            if phase == n_tp - 1:
                wide = jnp.concatenate([inv[...]] * (TILE // LANES), axis=1)
                pb[WINDOW:, cols] = (total * wide).astype(BF16)
            else:
                acc[:, cols] = total
            return carry

        lax.fori_loop(low, high, one, 0)

    gains.wait()
    load_tokens().wait()
    scaled(0)
    for i in range(4):
        load_weight(0, i).wait()
    project(0, 0, kv_tiles)
    for i in range(4, 6):
        load_weight(0, i).wait()
    for q in range(1, n_tp):
        for i in range(2):
            send_exit(q, i).start()
    for i in range(2):
        load_exit(i).start()
    project(0, kv_tiles, tiles)
    for phase in range(1, n_tp):
        for i in range(6):
            load_weight(phase, i).wait()
        send_tokens(n_tp - phase).wait_recv()
        scaled(phase)
        if phase < n_tp - 1:
            project(phase, 0, tiles)
    project(n_tp - 1, 0, kv_tiles)

    @pl.when(sp + 1 < n_sp)
    def _():
        send_halo().start()

    st[...] = jnp.zeros_like(st)

    def own_state(c, totals):
        span = pl.ds(pl.multiple_of(c * CHUNK, CHUNK), CHUNK)
        here = pl.ds(pl.multiple_of(WINDOW + c * CHUNK, CHUNK), CHUNK)
        after = []
        for p in range(pairs):
            cols = slice(p * LANES, (p + 1) * LANES)
            keys = pb[here, c_rk + p * LANES : c_rk + (p + 1) * LANES].astype(F32)
            values = pb[here, c_rv + p * LANES : c_rv + (p + 1) * LANES]
            keyed = (keys * ek[span, cols]).astype(BF16)
            added = lax.dot_general(keyed, values, TN, preferred_element_type=F32)
            added = jnp.where(same_head, added, 0.0)
            ub[c, p] = added
            fade = eq[span, cols][CHUNK - 1 :, :]
            st[p] = st[p] * fade + added
            after.append(totals[p] * fade)
        return tuple(after)

    totals = lax.fori_loop(
        0, chunks, own_state, tuple(jnp.ones((1, LANES), F32) for _ in range(pairs)),
        unroll=2,
    )
    for p in range(pairs):
        msg[p, :HEAD_DIM, :] = (st[p, :HEAD_DIM, :] + st[p, HEAD_DIM:, :]).astype(BF16)
        coarse = totals[p].astype(BF16)
        fine = (totals[p] - coarse.astype(F32)).astype(BF16)
        row16 = lax.broadcasted_iota(jnp.int32, (16, LANES), 0)
        msg[p, HEAD_DIM:, :] = jnp.where(
            row16 == 0, coarse.astype(F32), jnp.where(row16 == 1, fine.astype(F32), 0.0)
        ).astype(BF16)

    for q in range(1, n_sp):
        @pl.when(sp + q < n_sp)
        def _():
            send_state(q).start()

    project(n_tp - 1, kv_tiles, tiles)

    blocks = rows // WINDOW
    q_at = lax.broadcasted_iota(jnp.int32, (WINDOW, 2 * WINDOW), 0)
    k_at = lax.broadcasted_iota(jnp.int32, (WINDOW, 2 * WINDOW), 1)
    distance = WINDOW + q_at - k_at
    in_window = (distance >= 0) & (distance < WINDOW)

    def attend(i, carry):
        n = blocks - 1 - i

        lowest = jnp.where((n == 0) & (sp == 0), WINDOW, 0)
        allowed = in_window & (k_at >= lowest)
        band = pl.ds(pl.multiple_of(n * WINDOW, WINDOW), 2 * WINDOW)
        here = pl.ds(pl.multiple_of((n + 1) * WINDOW, WINDOW), WINDOW)
        store = pl.ds(pl.multiple_of(n * WINDOW, WINDOW), WINDOW)
        kinds = {}
        for t in range(kv_w // LANES):
            for name, col in (("k", c_ak), ("v", c_av)):
                plain = pb[band, col + t * LANES : col + (t + 1) * LANES]
                turned = pltpu.roll(plain.astype(F32), HEAD_DIM, 1).astype(BF16)
                kinds[name, t] = (plain, turned)
        scores = []
        picks = []
        for h in range(att_heads):
            p, e = h // 2, h % 2
            g = h * kv_heads // att_heads
            picks.append((g // 2, int(g % 2 != e)))
            query = pb[here, c_aq + p * LANES : c_aq + (p + 1) * LANES] * half_masks[e]
            t, turn = picks[h]
            scores.append(
                lax.dot_general(query, kinds["k", t][turn], NT, preferred_element_type=F32)
            )
        weights = []
        for h in range(att_heads):
            s = jnp.where(allowed, scores[h] * scale, -jnp.inf)
            sink_h = sink[h]
            highest = jnp.maximum(jnp.max(s, axis=1, keepdims=True), sink_h)
            raised = jnp.exp(s - highest)
            total = jnp.sum(raised, axis=1, keepdims=True) + jnp.exp(sink_h - highest)
            weights.append((raised * (1.0 / total)).astype(BF16))
        for p in range(att_pairs):
            left = jnp.concatenate([weights[2 * p], weights[2 * p + 1]], axis=1)
            right = jnp.concatenate(
                [
                    kinds["v", picks[2 * p + e][0]][picks[2 * p + e][1]] * half_masks[e]
                    for e in range(2)
                ],
                axis=0,
            )
            hb[store, ret_w + p * LANES : ret_w + (p + 1) * LANES] = jnp.dot(
                left, right, preferred_element_type=F32
            ).astype(BF16)
        return carry

    lax.fori_loop(0, blocks - 1, attend, 0)

    @pl.when(sp > 0)
    def _():
        send_halo().wait_recv()

    @pl.when(sp == 0)
    def _():
        pb[:WINDOW, c_ak : c_ak + 2 * kv_w] = jnp.zeros((WINDOW, 2 * kv_w), BF16)

    lax.fori_loop(blocks - 1, blocks, attend, 0)
    for q in range(1, n_tp):
        send_heads(q, 1).start()

    st[...] = jnp.zeros_like(st)
    for q in range(n_sp - 1, 0, -1):
        @pl.when(sp >= q)
        def _():
            send_state(q).wait_recv()
            for p in range(pairs):
                part = inbox[q - 1, p].astype(F32)
                fade = part[HEAD_DIM : HEAD_DIM + 1] + part[HEAD_DIM + 1 : HEAD_DIM + 2]
                both = jnp.concatenate([part[:HEAD_DIM]] * 2, axis=0)
                st[p] = st[p] * fade + jnp.where(same_head, both, 0.0)

    ones = jnp.where(same_head, 1.0, 0.0).astype(BF16)
    ones2 = jnp.concatenate([ones, ones], axis=0)

    def retain(c, carry):
        span = pl.ds(pl.multiple_of(c * CHUNK, CHUNK), CHUNK)
        here = pl.ds(pl.multiple_of(WINDOW + c * CHUNK, CHUNK), CHUNK)
        kept = []
        for p in range(pairs):
            cols = slice(p * LANES, (p + 1) * LANES)
            query = pb[here, c_rq + p * LANES : c_rq + (p + 1) * LANES]
            keys = pb[here, c_rk + p * LANES : c_rk + (p + 1) * LANES]
            values = pb[here, c_rv + p * LANES : c_rv + (p + 1) * LANES]
            left = [
                (
                    lax.dot_general(
                        query * half_masks[e], keys, NT, preferred_element_type=F32
                    )
                    * dm[c, 2 * p + e]
                ).astype(BF16)
                for e in range(2)
            ]
            state = st[p]
            faded = eq[span, cols]
            left.append((query.astype(F32) * faded).astype(BF16))
            right = [values * half_masks[0], values * half_masks[1], state.astype(BF16)]
            kept.append(
                jnp.dot(
                    jnp.concatenate(left, axis=1),
                    jnp.concatenate(right, axis=0),
                    preferred_element_type=F32,
                )
            )
            st[p] = state * faded[CHUNK - 1 :, :] + ub[c, p]
        for p in range(pairs):
            cols = slice(p * LANES, (p + 1) * LANES)
            r = kept[p]
            square = r * r
            coarse = square.astype(BF16)
            fine = (square - coarse.astype(F32)).astype(BF16)
            total = jnp.dot(
                jnp.concatenate([coarse, fine], axis=1), ones2, preferred_element_type=F32
            )
            normed = r * lax.rsqrt(total * (1.0 / HEAD_DIM) + EPS)
            hb[span, cols] = (normed * rgain[cols].reshape(1, LANES)).astype(BF16)
        return carry

    lax.fori_loop(0, chunks, retain, 0, unroll=2)
    for q in range(1, n_tp):
        send_heads(q, 0).start()

    for i in range(2):
        load_exit(i).wait()
    mine = pl.ds(pl.multiple_of(tp * out_rows, out_rows), out_rows)

    def leave(phase):
        def one(n, carry):
            cols = pl.ds(pl.multiple_of(n * EXIT_TILE, EXIT_TILE), EXIT_TILE)
            left = hb[mine, :] if phase == 0 else hin[phase - 1]
            total = jnp.dot(left, wo[phase, :, cols], preferred_element_type=F32)
            if phase > 0:
                total = oacc[:, cols] + total
            if phase == n_tp - 1:
                out[:, cols] = total.astype(BF16)
            else:
                oacc[:, cols] = total
            return carry

        lax.fori_loop(0, model // EXIT_TILE, one, 0)

    leave(0)
    for phase in range(1, n_tp):
        for i in range(2):
            send_exit(n_tp - phase, i).wait_recv()
            send_heads(n_tp - phase, i).wait_recv()
        leave(phase)

    for q in range(1, n_tp):
        send_tokens(q).wait_send()
        for i in range(2):
            send_exit(q, i).wait_send()
            send_heads(q, i).wait_send()
    for q in range(1, n_sp):
        @pl.when(sp + q < n_sp)
        def _():
            send_state(q).wait_send()

    @pl.when(sp + 1 < n_sp)
    def _():
        send_halo().wait_send()


def shards(n_sp, n_tp, tokens, in_gain, rq, rk, rv, aq, ak, av, log_decay, ret_gain, sink, wr, wa):
    rows, depth = tokens.shape[1:]
    ret_w, att_w, kv_w = rq.shape[1], aq.shape[1], ak.shape[1]
    heads = log_decay.shape[1]
    model = depth * n_tp
    width = 3 * ret_w + att_w + 2 * kv_w
    chunks, pairs = rows // CHUNK, ret_w // LANES
    out_rows = rows // n_tp
    kv_heads = kv_w // HEAD_DIM
    later = max(n_sp - 1, 1)
    others = max(n_tp - 1, 1)
    vmem = pl.BlockSpec(memory_space=pltpu.VMEM)
    hbm = pl.BlockSpec(memory_space=pltpu.HBM)
    smem = pl.BlockSpec(memory_space=pltpu.SMEM)
    dma = pltpu.SemaphoreType.DMA
    result = pl.pallas_call(
        functools.partial(layer, n_sp, n_tp, kv_heads),
        out_shape=pltpu.VMEM((out_rows, model), BF16),
        in_specs=[hbm] * 9 + [vmem, smem, hbm, hbm],
        out_specs=vmem,
        scratch_shapes=[
            pltpu.VMEM((n_tp, rows, depth), BF16),
            pltpu.VMEM((n_tp, depth, width), BF16),
            pltpu.VMEM((rows, width), F32),
            pltpu.VMEM((WINDOW + rows, width), BF16),
            pltpu.VMEM((rows, LANES), F32),
            pltpu.VMEM((LANES, rows), F32),
            pltpu.VMEM((rows, LANES), F32),
            pltpu.VMEM((chunks, 8, CHUNK), F32),
            pltpu.VMEM((rows, ret_w), F32),
            pltpu.VMEM((rows, ret_w), F32),
            pltpu.VMEM((chunks, heads, CHUNK, CHUNK), F32),
            pltpu.VMEM((pairs, LANES, LANES), F32),
            pltpu.VMEM((chunks, pairs, LANES, LANES), F32),
            pltpu.VMEM((pairs, HEAD_DIM + 16, LANES), BF16),
            pltpu.VMEM((later, pairs, HEAD_DIM + 16, LANES), BF16),
            pltpu.VMEM((rows, ret_w + att_w), BF16),
            pltpu.VMEM((others, out_rows, ret_w + att_w), BF16),
            pltpu.VMEM((n_tp, ret_w + att_w, model), BF16),
            pltpu.VMEM((out_rows, model), F32),
            pltpu.VMEM((n_tp, 1, depth), F32),
            pltpu.VMEM((heads, 1, rows), F32),
            dma((2,)),
            dma, dma((n_tp, 6)), dma((2,)),
            dma((others,)), dma((others,)),
            dma((others, 2)), dma((others, 2)),
            dma((others, 2)), dma((others, 2)),
            dma((later,)), dma((later,)),
            dma, dma,
        ],
        compiler_params=pltpu.CompilerParams(
            collective_id=0, has_side_effects=True, vmem_limit_bytes=52 * 1024 * 1024
        ),
    )(
        tokens[0], in_gain.reshape(n_tp, 1, depth), rq, rk, rv, aq, ak, av,
        jnp.transpose(log_decay, (1, 0, 2)), ret_gain, sink, wr, wa,
    )
    return result[None]


def solution(mesh):
    n_sp, n_tp = mesh.shape["sp"], mesh.shape["tp"]
    return jax.shard_map(
        functools.partial(shards, n_sp, n_tp),
        mesh=mesh,
        in_specs=(
            P("fs", "sp", "tp"),
            P(),
            P(None, "tp"),
            P(None, "tp"),
            P(None, "tp"),
            P(None, "tp"),
            P(None, "tp"),
            P(None, "tp"),
            P("fs", "tp", "sp"),
            P("tp"),
            P("tp"),
            P("tp", None),
            P("tp", None),
        ),
        out_specs=P("fs", ("sp", "tp"), None),
        check_vma=False,
    )
```
